32 devices in a mesh: kv: 8 (over y, x, core), tp: 4 (over z).
Axes of the slice: x: 2, y: 2, z: 4, core: 2. Of those that a mesh axis runs over, the one named last changes fastest.
Arguments:
- tokens: bfloat16 [320, 4096], P('tp', 'kv'), may hold values from -8 to 8
- state: float32 [320, 32, 128, 128], P('kv', 'tp'), may hold values from -4 to 4
- mix_gain: float32 [4096], P('kv'), may hold values from 0.1 to 1.9
- q_weight: bfloat16 [4096, 4096], P('kv', 'tp'), may hold values from -0.09375 to 0.09375
- forget_weight: bfloat16 [4096, 4096], P('kv', 'tp'), may hold values from -0.09375 to 0.09375
- input_weight: bfloat16 [4096, 4096], P('kv', 'tp'), may hold values from -0.09375 to 0.09375
- gate_weight: bfloat16 [4096, 4096], P('kv', 'tp'), may hold values from -0.09375 to 0.09375
- lower_bound: float32 [4096], P('tp'), may hold values from 0 to 0.9
- head_gain: float32 [128], replicated, may hold values from 0.1 to 1.9
- out_weight: bfloat16 [4096, 4096], P('tp', 'kv'), may hold values from -0.09375 to 0.09375
- ffn_gain: float32 [4096], P('kv'), may hold values from 0.1 to 1.9
- ffn_gate: bfloat16 [4096, 10240], P('kv', 'tp'), may hold values from -0.09375 to 0.09375
- ffn_up: bfloat16 [4096, 10240], P('kv', 'tp'), may hold values from -0.09375 to 0.09375
- ffn_down: bfloat16 [10240, 4096], P('tp', 'kv'), may hold values from -0.0625 to 0.0625
Outputs:
- layer_out: bfloat16 [320, 4096], P('tp', 'kv')
- new_state: float32 [320, 32, 128, 128], P('kv', 'tp')
The draws below stay inside these ranges and needn't reach their ends.
All inputs are finite; a program needn't handle non-finite values.
Results may differ from the reference program's by a relative error of at most 0.007.
Values may be sent and summed in bfloat16 or wider, within the bound.
A program may use at most 128 MiB of HBM per device.

```python
import jax
import jax.numpy as jnp
from jax import lax

HEADS = 32
HEAD = 128
D = 4096
FF = 10240
BATCH = 320


def draw_tokens(key, part):
    first, second, third, fourth = jax.random.split(jax.random.fold_in(key, 17), 4)
    base = jax.random.normal(first, (BATCH, D), jnp.float32)
    block_scale = jnp.exp(jax.random.uniform(second, (32,), jnp.float32, -1.2, 1.2))
    column_scale = jnp.repeat(block_scale, D // 32)
    values = base * column_scale[None, :]
    return jnp.clip(values, -8.0, 8.0).astype(jnp.bfloat16)


def levels(stream_key, shape, cuts, least, top_value):
    def one(axis_at, parts):
        draws = jax.random.uniform(jax.random.fold_in(jax.random.fold_in(stream_key, 6), axis_at), (parts,), jnp.float32, least / len(cuts), top_value / len(cuts))
        return jnp.repeat(jnp.exp(draws), shape[axis_at] // parts).reshape((-1,) + (1,) * (len(shape) - axis_at - 1))

    loudness = one(*cuts[0])
    for cut in cuts[1:]:
        loudness = loudness * one(*cut)
    return loudness


def gaussian(key, shape, scale, bound, shards=(), kind=jnp.bfloat16):
    array = scale * jax.random.normal(key, shape, jnp.float32)
    if shards:
        array = array * levels(key, shape, shards, -0.22, 0.18)
    return jnp.clip(array, -bound, bound).astype(kind)


def setup_inputs(seed: int = 0) -> dict:
    key_of = jax.random.split(jax.random.key(seed), 15)
    tokens = draw_tokens(jax.random.fold_in(key_of[14], 71), 0)
    state = gaussian(key_of[1], (BATCH, HEADS, HEAD, HEAD), 0.5, 4.0, ((0, 8), (1, 4)), jnp.float32)
    mix_gain = jnp.clip(1.0 + 0.18 * jax.random.normal(key_of[2], (D,), jnp.float32), 0.1, 1.9)
    q_weight = gaussian(key_of[3], (D, D), D ** -0.5, 0.09375, ((0, 8), (1, 4)))
    forget_weight = gaussian(key_of[4], (D, D), D ** -0.5, 0.09375, ((0, 8), (1, 4)))
    input_weight = gaussian(key_of[5], (D, D), D ** -0.5, 0.09375, ((0, 8), (1, 4)))
    gate_weight = gaussian(key_of[6], (D, D), D ** -0.5, 0.09375, ((0, 8), (1, 4)))
    lower_bound = jnp.clip(0.9 * jax.random.uniform(key_of[7], (D,), jnp.float32) ** levels(key_of[7], (D,), ((0, 4),), -0.2, 0.2), 0.0, 0.9)
    head_gain = jnp.clip(1.0 + 0.18 * jax.random.normal(key_of[8], (HEAD,), jnp.float32), 0.1, 1.9)
    out_weight = gaussian(key_of[9], (D, D), D ** -0.5, 0.09375, ((0, 4), (1, 8)))
    ffn_gain = jnp.clip(1.0 + 0.18 * jax.random.normal(key_of[10], (D,), jnp.float32), 0.1, 1.9)
    ffn_gate = gaussian(key_of[11], (D, FF), D ** -0.5, 0.09375, ((0, 8), (1, 4)))
    ffn_up = gaussian(key_of[12], (D, FF), D ** -0.5, 0.09375, ((0, 8), (1, 4)))
    ffn_down = gaussian(key_of[13], (FF, D), FF ** -0.5, 0.0625, ((0, 4), (1, 8)))
    return {"tokens": tokens, "state": state, "mix_gain": mix_gain, "q_weight": q_weight, "forget_weight": forget_weight, "input_weight": input_weight, "gate_weight": gate_weight, "lower_bound": lower_bound, "head_gain": head_gain, "out_weight": out_weight, "ffn_gain": ffn_gain, "ffn_gate": ffn_gate, "ffn_up": ffn_up, "ffn_down": ffn_down}


EPS = 1e-05

def reference(tokens, state, mix_gain, q_weight, forget_weight, input_weight, gate_weight, lower_bound, head_gain, out_weight, ffn_gain, ffn_gate, ffn_up, ffn_down):
    batch_rows = tokens.shape[0]
    values = tokens.astype(jnp.float32)
    factor = lax.rsqrt(lax.optimization_barrier(jnp.mean(values * values, axis=1, keepdims=True)) + EPS)
    normed = (values * mix_gain).astype(jnp.bfloat16)

    def project(weight):
        return jnp.dot(normed, weight, preferred_element_type=jnp.float32) * factor
    query_pre = project(q_weight)
    forget_pre = project(forget_weight)
    value_pre = project(input_weight)
    gate_pre = project(gate_weight)
    split_shape = (batch_rows, HEADS, HEAD)
    query = (jax.nn.silu(query_pre) * HEAD ** (-0.5)).reshape(split_shape)
    forget = (lower_bound + (1.0 - lower_bound) * jax.nn.sigmoid(forget_pre)).reshape(split_shape)
    value = value_pre.reshape(split_shape)
    new_state = forget[..., None] * state + (1.0 - forget)[..., None] * value[:, :, None, :]
    read = jnp.einsum('bhk,bhkv->bhv', query, new_state, precision=lax.Precision.HIGHEST)
    read = read * lax.rsqrt(lax.optimization_barrier(jnp.mean(read * read, axis=-1, keepdims=True)) + EPS) * head_gain
    gated = (read.reshape(batch_rows, D) * jax.nn.silu(gate_pre)).astype(jnp.bfloat16)
    residual = (values + jnp.dot(gated, out_weight, preferred_element_type=jnp.float32)).astype(jnp.bfloat16)
    res_values = residual.astype(jnp.float32)
    factor_ffn = lax.rsqrt(lax.optimization_barrier(jnp.mean(res_values * res_values, axis=1, keepdims=True)) + EPS)
    normed_ffn = (res_values * ffn_gain).astype(jnp.bfloat16)
    gate_ffn = jnp.dot(normed_ffn, ffn_gate, preferred_element_type=jnp.float32) * factor_ffn
    up_ffn = jnp.dot(normed_ffn, ffn_up, preferred_element_type=jnp.float32) * factor_ffn
    hidden = (jax.nn.silu(gate_ffn) * up_ffn).astype(jnp.bfloat16)
    layer_out = (res_values + jnp.dot(hidden, ffn_down, preferred_element_type=jnp.float32)).astype(jnp.bfloat16)
    return (layer_out, new_state)
```

```python
import functools

import jax
import jax.numpy as jnp
from jax import lax
from jax.experimental import pallas as pl
from jax.experimental.pallas import tpu as pltpu
from jax.sharding import PartitionSpec as P

EPS = 1e-05
F32 = jnp.float32
BF16 = jnp.bfloat16
LANES = 128
SUB = 8
SLOTS = 3
MESH = pl.DeviceIdType.MESH
ANY = pl.BlockSpec(memory_space=pl.ANY)
VMEM = pl.BlockSpec(memory_space=pltpu.VMEM)


def greet(n_kv, n_tp):
    kv, tp = lax.axis_index("kv"), lax.axis_index("tp")
    barrier = pltpu.get_barrier_semaphore()
    for axis, me, n in (("kv", kv, n_kv), ("tp", tp, n_tp)):
        for off in range(1, n):
            pl.semaphore_signal(
                barrier,
                inc=1,
                device_id={axis: lax.rem(me + off, n)},
                device_id_type=MESH,
            )
    pl.semaphore_wait(barrier, n_kv + n_tp - 2)


PLANS = {
    5: (
        (1, 1, 1, 1, 1),
        (
            0, 1, 0, 2, 1, 3, 2, 4, 0, 1, 3, 0, 2, 1, 3, 0, 4, 2, 0, 1, 1, 3, 4, 2,
            0, 2, 3, 1, 0, 4, 3, 0, 2, 1, 1, 3, 4, 2, 0, 4, 2, 1, 4, 0, 2, 3, 1, 0,
            3, 4, 4, 3, 1, 2, 4, 1, 3, 0, 4, 2, 3, 2, 4, 0, 1, 3, 4, 3, 2, 4,
        ),
    ),
}


def groups_of(rows):
    if rows % SUB:
        return [(0, rows)]
    parts = PLANS[rows // SUB][0] if rows // SUB in PLANS else (rows // SUB,)
    return [(SUB * sum(parts[:i]), SUB * part) for i, part in enumerate(parts)]


def order_of(groups):
    sizes = tuple(size // SUB for _, size in groups)
    for parts, order in PLANS.values():
        if parts == sizes:
            return order
    return [i for _ in range(STEPS) for i in range(len(groups))]


STEPS = 15


def tile_of(cols):
    return next((t for t in (512, 640, 384, 256, 128) if cols % t == 0), cols)


class Layer:
    def __init__(self, dims, refs):
        self.__dict__.update(dims)
        self.__dict__.update(refs)
        self.kv = lax.axis_index("kv")
        self.tp = lax.axis_index("tp")
        self.par = lax.rem(self.kv, 2)
        self.chip = self.kv // 2
        self.partner = self.kv + 1 - 2 * self.par
        self.half = self.n_kv // 2
        self.near = (self.chip + 1 - 2 * lax.rem(self.chip, 2), lax.rem(self.chip + 2, 4))
        self.started = []
        self.sems = {}
        self.used = 0
        self.state_at = {}

    def remote(self, src, dst, axis, peer):
        i = self.used
        self.used += 1
        copy = pltpu.make_async_remote_copy(
            src_ref=src,
            dst_ref=dst,
            send_sem=self.send.at[i],
            recv_sem=self.recv.at[i],
            device_id={axis: peer},
            device_id_type=MESH,
        )
        copy.start()
        self.started.append(copy)
        return copy


    def tp_start(self, src, into, rows):
        copies = []
        for off in range(1, self.n_tp):
            peer = lax.rem(self.tp + off, self.n_tp)
            copies.append(self.remote(src, into.at[self.par, self.tp, :, rows], "tp", peer))
        pair = self.remote(src, into.at[self.par, self.tp, :, rows], "kv", self.partner)
        into[self.par, self.tp, :, rows] = src[...]
        return copies, [pair]

    def tp_relay(self, moved, into, rows):
        copies, pairs = moved
        for off in range(1, self.n_tp):
            copies[off - 1].wait_recv()
            source = lax.rem(self.tp + self.n_tp - off, self.n_tp)
            block = into.at[self.par, source, :, rows]
            pairs.append(self.remote(block, block, "kv", self.partner))


    def kv_start(self, src, into, rows):
        copies = []
        for off in range(1, self.half):
            peer = lax.rem(self.chip + off, self.half) * 2 + self.par
            copies.append(self.remote(src, into.at[self.kv, rows], "kv", peer))
        pair = self.remote(src, into.at[self.kv, rows], "kv", self.partner)
        into[self.kv, rows] = src[...]
        return copies, [pair]

    def kv_relay(self, moved, into, rows):
        copies, pairs = moved
        for off in range(1, self.half):
            copies[off - 1].wait_recv()
            source = lax.rem(self.chip + self.half - off, self.half) * 2 + self.par
            block = into.at[source, rows]
            pairs.append(self.remote(block, block, "kv", self.partner))


    def spread(self, out, into, passing, rows):
        copies = [self.remote(out.at[self.partner, rows], into.at[self.kv, rows], "kv", self.partner)]
        passed = []
        if self.square:
            ways = list(zip(self.near, self.halves(out)))
            far = pl.ds(2 * (self.half - 1 - self.chip), 2)
            for k, (chip, cols) in enumerate(ways):
                peer = 2 * chip + self.par
                passed.append(
                    self.remote(out.at[far, rows, cols], passing.at[k, :, rows], "kv", peer)
                )
            for chip, cols in ways:
                for peer in (2 * chip + self.par, 2 * chip + 1 - self.par):
                    to = into.at[self.kv, rows, cols]
                    copies.append(self.remote(out.at[peer, rows, cols], to, "kv", peer))
        else:
            for off in range(1, self.half):
                chip = lax.rem(self.chip + off, self.half) * 2
                for peer in (chip + self.par, chip + 1 - self.par):
                    copies.append(self.remote(out.at[peer, rows], into.at[self.kv, rows], "kv", peer))
        into[self.kv, rows] = out[self.kv, rows]
        return copies, passed

    def spread_on(self, sent, out, into, passing, rows):
        copies, passed = sent
        ways = list(zip(self.near[::-1], self.halves(out)))
        for k, (chip, cols) in enumerate(ways):
            passed[k].wait_recv()
            for q in range(2):
                total = out[2 * chip + q, rows, cols].astype(F32)
                out[2 * chip + q, rows, cols] = (
                    total + passing[k, q, rows].astype(F32)
                ).astype(BF16)
            for peer in (2 * chip + self.par, 2 * chip + 1 - self.par):
                to = into.at[self.kv, rows, cols]
                copies.append(self.remote(out.at[peer, rows, cols], to, "kv", peer))

    def halves(self, out):
        wide = out.shape[2] // 2
        return pl.ds(0, wide), pl.ds(wide, wide)

    def collect(self, into, rows, parity, cols):
        if self.square:
            total = into[2 * self.chip + parity, rows, cols].astype(F32)
            for chip in self.near:
                total = total + into[2 * chip + parity, rows, cols].astype(F32)
            return total
        total = into[parity, rows, cols].astype(F32)
        for i in range(1, self.half):
            total = total + into[2 * i + parity, rows, cols].astype(F32)
        return total

    def factor(self, copies, into, rows):
        for copy in copies:
            copy.wait_recv()
        total = into[0, rows]
        for i in range(1, self.half):
            total = total + into[i, rows]
        return lax.rsqrt(total[:, :1] / self.width + EPS)


    def terms_start(self, k, product, rows, size):
        product = product.reshape(self.n_tp, self.g, size, self.feats)
        self.t_acc[k, :, :, rows] = product
        self.t_out[k, :, :, rows] = product.astype(BF16)
        copies = []
        for off in range(1, self.n_tp):
            peer = lax.rem(self.tp + off, self.n_tp)
            copies.append(
                self.remote(
                    self.t_out.at[k, peer, :, rows], self.t_in.at[k, self.tp, :, rows], "tp", peer
                )
            )
        return copies

    def terms_total(self, k, copies, rows):
        total = self.t_acc[k, self.tp, :, rows]
        for off in range(1, self.n_tp):
            copies[off - 1].wait_recv()
            source = lax.rem(self.tp + self.n_tp - off, self.n_tp)
            total = total + self.t_in[k, source, :, rows].astype(F32)
        return total


    def load(self, i, src, dst):
        copy = pltpu.make_async_copy(src, dst, self.load_sem.at[i])
        copy.start()
        return copy

    def pair_load_local(self, weights, dst, at):
        mine = pl.ds(self.par * self.feats, self.feats)
        n = len(weights) // 2
        for p in range(2):

            @pl.when(self.par == p)
            def _(p=p):
                for i in range(n):
                    self.load(at + i, weights[p * n + i], dst.at[i, mine])

        return [
            pltpu.make_async_copy(weights[i], dst.at[i, mine], self.load_sem.at[at + i])
            for i in range(n)
        ]

    def pair_load_remote(self, weights, dst):
        mine = pl.ds(self.par * self.feats, self.feats)
        n = len(weights) // 2
        at = self.used
        self.used += n

        def copy(p, i):
            return pltpu.make_async_remote_copy(
                src_ref=weights[(1 - p) * n + i],
                dst_ref=dst.at[i, mine],
                send_sem=self.send.at[at + i],
                recv_sem=self.recv.at[at + i],
                device_id={"kv": self.partner},
                device_id_type=MESH,
            )

        for p in range(2):

            @pl.when(self.par == p)
            def _(p=p):
                for i in range(n):
                    copy(p, i).start()

        waits = [copy(0, i) for i in range(n)]
        self.started.extend(waits)
        return waits

    def state_load(self, c):
        slot = c % SLOTS
        rows = pl.ds(c * self.chunk, self.chunk)
        copy = pltpu.make_async_copy(
            self.state.at[rows], self.s_buf.at[slot], self.state_sem.at[slot]
        )
        copy.start()
        self.state_at[c] = copy


    def normed(self, into, rows, size):
        total = self.n_kv * size
        squares = None
        for p in range(2):
            values = into[p, :, :, rows].astype(F32).reshape(total, self.feats)
            cols = pl.ds(p * self.feats, self.feats)
            self.lhs[:total, cols] = (values * self.gains[self.which, p]).astype(BF16)
            part = jnp.sum(values * values, axis=1, keepdims=True)
            squares = part if squares is None else squares + part
        return squares

    def project(self, weights, cols, out, rows, size):
        total = self.n_kv * size
        tile = tile_of(cols)
        per = cols // tile
        n = weights.shape[0]

        def step(t, carry):
            i, at = t // per, pl.multiple_of(lax.rem(t, per) * tile, LANES)
            product = jnp.dot(
                self.lhs[:total, :], weights[i, :, pl.ds(at, tile)], preferred_element_type=F32
            )
            to = pl.multiple_of(t * tile, LANES)
            out[:, rows, pl.ds(to, tile)] = product.reshape(self.n_kv, size, tile).astype(BF16)
            return carry

        [step(t, 0) for t in range(n * per)]

    def flat(self, block, size):
        return block.astype(F32).reshape(self.n_kv * size, block.shape[2]).astype(BF16)

    def read_state(self, rows, size):
        n = self.head_size
        shape = (self.heads, self.heads * n)
        own = lax.broadcasted_iota(jnp.int32, shape, 0) == (
            lax.broadcasted_iota(jnp.int32, shape, 1) // n
        )
        for c in range(rows.start // self.chunk, (rows.start + size) // self.chunk):
            self.state_at[c].wait()
            slot = c % SLOTS
            here = pl.ds(c * self.chunk, self.chunk)

            for b in range(self.chunk):
                at = pl.ds(c * self.chunk + b, 1)
                qf = self.qf[at]
                high = qf.astype(BF16).astype(F32)
                parts = jnp.concatenate(
                    [jnp.where(own, high, 0.0), jnp.where(own, qf - high, 0.0)], axis=0
                )
                kept = self.s_buf[slot, b].reshape(self.heads * n, n).astype(BF16)
                seen = jnp.dot(parts.astype(BF16), kept, preferred_element_type=F32)
                self.seen[at] = (seen[: self.heads] + seen[self.heads :])[None]
            if c + SLOTS < self.chunks:
                self.state_load(c + SLOTS)
        for h in range(self.heads):
            cols = pl.ds(h * n, n)
            rest = jnp.sum(self.qv[rows, cols], axis=1, keepdims=True)
            seen = self.seen[rows, h] + rest * self.fv[1, rows, cols]
            seen = seen * lax.rsqrt(jnp.mean(seen * seen, axis=1, keepdims=True) + EPS)
            seen = seen * self.head_gain[...]
            self.gated[rows, cols] = (seen * self.opened[rows, cols]).astype(BF16)


    def stages(self, rows, size):
        cols = self.cols
        tokens_at = self.tokens.at[:, rows]

        moved = self.tp_start(tokens_at, self.x_all, rows)
        yield
        self.tp_relay(moved, self.x_all, rows)
        yield
        for copy in moved[1]:
            copy.wait_recv()
        self.ready("mixer")
        self.which = 0
        squares = self.normed(self.x_all, rows, size)
        self.project(self.w_mix, cols, self.m_out, rows, size)
        sent = self.spread(self.m_out, self.m_in, self.m_pass, rows)
        summed = self.squares_send(squares, 0, rows, size)
        yield
        self.then("mixer")
        if self.square:
            self.spread_on(sent, self.m_out, self.m_in, self.m_pass, rows)
            yield
        for copy in sent[0]:
            copy.wait_recv()
        factor = self.factor(summed, self.q_in.at[0], rows)
        low = self.low[...]
        size_k = self.head_size
        first, second = pl.ds(0, cols), pl.ds(cols, cols)
        query = jax.nn.silu(self.collect(self.m_in, rows, 0, first) * factor) * size_k ** (-0.5)
        forget = low + (1.0 - low) * jax.nn.sigmoid(
            self.collect(self.m_in, rows, 0, second) * factor
        )
        self.fv[0, rows] = forget
        self.qf[rows] = query * forget
        self.qv[rows] = query * (1.0 - forget)
        self.fv[1, rows] = self.collect(self.m_in, rows, 1, first) * factor
        self.opened[rows] = jax.nn.silu(self.collect(self.m_in, rows, 1, second) * factor)
        self.read_state(rows, size)
        moved = self.kv_start(self.gated.at[rows], self.g_all, rows)
        yield
        self.kv_relay(moved, self.g_all, rows)
        yield
        for copy in moved[1]:
            copy.wait_recv()
        self.ready("out")
        product = jnp.dot(
            self.flat(self.g_all[:, rows], size), self.w_out_v[...], preferred_element_type=F32
        )
        terms = self.terms_start(0, product, rows, size)
        yield
        attended = self.terms_total(0, terms, rows)
        self.res[:, rows] = (self.tokens[:, rows].astype(F32) + attended).astype(BF16)
        moved = self.tp_start(self.res.at[:, rows], self.r_all, rows)
        yield
        self.tp_relay(moved, self.r_all, rows)
        yield
        for copy in moved[1]:
            copy.wait_recv()
        self.ready("ffn")
        self.which = 1
        squares = self.normed(self.r_all, rows, size)
        self.project(self.w_ffn, self.ff, self.f_out, rows, size)
        sent = self.spread(self.f_out, self.f_in, self.f_pass, rows)
        summed = self.squares_send(squares, 1, rows, size)
        yield
        if self.square:
            self.spread_on(sent, self.f_out, self.f_in, self.f_pass, rows)
            yield
        for copy in sent[0]:
            copy.wait_recv()
        factor = self.factor(summed, self.q_in.at[1], rows)
        every = pl.ds(0, self.ff)
        gate = self.collect(self.f_in, rows, 0, every) * factor
        up = self.collect(self.f_in, rows, 1, every) * factor
        self.hid[rows] = (jax.nn.silu(gate) * up).astype(BF16)
        moved = self.kv_start(self.hid.at[rows], self.h_all, rows)
        yield
        self.kv_relay(moved, self.h_all, rows)
        yield
        for copy in moved[1]:
            copy.wait_recv()
        self.ready("down")
        product = jnp.dot(
            self.flat(self.h_all[:, rows], size), self.w_down_v[...], preferred_element_type=F32
        )
        terms = self.terms_start(1, product, rows, size)
        yield
        down = self.terms_total(1, terms, rows)
        self.out[:, rows] = (self.res[:, rows].astype(F32) + down).astype(BF16)

    def squares_send(self, totals, k, rows, size):
        out, into = self.q_out.at[k], self.q_in.at[k]
        totals = jnp.broadcast_to(totals, (self.n_kv * size, LANES))
        out[:, rows] = totals.reshape(self.n_kv, size, LANES)
        copies = []
        for off in range(1, self.half):
            peer = lax.rem(self.chip + off, self.half) * 2 + self.par
            copies.append(self.remote(out.at[peer, rows], into.at[self.chip, rows], "kv", peer))
        into[self.chip, rows] = out[self.kv, rows]
        return copies

    def ready(self, name):
        for copy in self.pending.pop(name, ()):
            if isinstance(copy, tuple):
                copy[0].wait_recv()
            else:
                copy.wait()

    def then(self, name):
        for start in self.later.pop(name, ()):
            start()


NAMES = (
    "tokens", "mix_gain", "ffn_gain", "low", "head_gain", "state", "wq", "wf", "wv", "wg",
    "w_out", "w_gate", "w_up", "w_down", "out", "fv", "w_mix", "w_ffn", "w_out_v", "w_down_v",
    "x_all", "r_all", "lhs", "gains", "m_out", "m_in", "f_out", "f_in", "m_pass", "f_pass", "q_out", "q_in", "qf",
    "qv", "seen", "opened", "gated", "g_all", "hid", "h_all", "t_acc", "t_out", "t_in", "res",
    "s_buf", "send", "recv", "load_sem", "state_sem",
)


def layer(dims, *refs):
    run = Layer(dims, dict(zip(NAMES, refs)))
    mix = (run.wq, run.wf, run.wv, run.wg)
    ffn = (run.w_gate, run.w_up)
    local_mix = run.pair_load_local(mix, run.w_mix, 0)
    for c in range(min(SLOTS, run.chunks)):
        run.state_load(c)
    local_out = run.load(2, run.w_out, run.w_out_v)
    local_ffn = run.pair_load_local(ffn, run.w_ffn, 3)
    local_down = run.load(4, run.w_down, run.w_down_v)
    greet(run.n_kv, run.n_tp)
    run.pending = {
        "out": [local_out],
        "down": [local_down],
        "mixer": list(local_mix),
        "ffn": list(local_ffn),
    }

    def share_gain(k, gain):
        run.gains[k, run.par] = gain[...]
        copy = run.remote(gain, run.gains.at[k, run.par], "kv", run.partner)
        run.pending[("mixer", "ffn")[k]].append((copy,))

    def share_ffn():
        for copy in run.pair_load_remote(ffn, run.w_ffn):
            run.pending["ffn"].append((copy,))

    run.later = {"mixer": [share_ffn]}
    flows = [run.stages(pl.ds(at, size), size) for at, size in dims["groups"]]
    live = {i: 0 for i in range(len(flows))}
    for flow in flows:
        next(flow)
    share_gain(0, run.mix_gain)
    share_gain(1, run.ffn_gain)
    for copy in run.pair_load_remote(mix, run.w_mix):
        run.pending["mixer"].append((copy,))
    for i in dims["order"]:
        next(flows[i], None)
    for copy in run.started:
        copy.wait_send()


def state_step(fv, layer_in, state, new_state, layer_out):
    n, heads, size = state.shape[:3]
    shape = (3 * n, n * size)
    own = lax.rem(lax.broadcasted_iota(jnp.int32, shape, 0), n) == (
        lax.broadcasted_iota(jnp.int32, shape, 1) // size
    )
    pick = jnp.where(own, 1.0, 0.0).astype(BF16)
    layer_out[...] = layer_in[...]
    for h in range(heads):
        cols = slice(h * size, (h + 1) * size)
        forget = fv[0, :, cols]
        high = forget.astype(BF16).astype(F32)
        middle = (forget - high).astype(BF16).astype(F32)
        parts = jnp.concatenate([high, middle, forget - high - middle], axis=0)
        wide = lax.dot_general(
            parts.astype(BF16), pick, (((0,), (0,)), ((), ())), preferred_element_type=F32
        )
        for b in range(n):
            v = fv[1, b : b + 1, cols]
            keep = wide[:, b * size : (b + 1) * size]
            new_state[b, h] = v + keep * (state[b, h] - v)


def body(
    n_kv,
    n_tp,
    tokens,
    state,
    mix_gain,
    q_weight,
    forget_weight,
    input_weight,
    gate_weight,
    lower_bound,
    head_gain,
    out_weight,
    ffn_gain,
    ffn_gate,
    ffn_up,
    ffn_down,
):
    rows_tp, feats = tokens.shape
    rows, heads, size = state.shape[:3]
    cols = q_weight.shape[1]
    ff = ffn_gate.shape[1]
    g = rows_tp // rows
    groups = groups_of(rows)
    most = max(s for _, s in groups)
    chunk = SUB if rows % SUB == 0 else rows
    half = n_kv // 2
    square = half == 4 and cols % LANES == 0 and ff % (2 * LANES) == 0
    dims = dict(
        square=square,
        n_kv=n_kv,
        n_tp=n_tp,
        width=feats * n_kv,
        feats=feats,
        rows=rows,
        heads=heads,
        head_size=size,
        cols=cols,
        ff=ff,
        g=g,
        groups=groups,
        order=order_of(groups),
        chunk=chunk,
        chunks=rows // chunk,
    )
    per_group = 2 * n_tp + 2 * n_kv + 2 * (n_tp - 1) + 2 * half + 2 * (n_kv - 1) + 2 * n_tp + 24
    n_sems = per_group * len(groups) + 8
    dma = pltpu.SemaphoreType.DMA
    tiny = tokens.reshape(g, rows, feats)
    held = [
        pltpu.with_memory_space_constraint(x, pltpu.HBM)
        for x in (
            tiny,
            mix_gain[None, :],
            ffn_gain[None, :],
            lower_bound[None, :],
            head_gain[None, :],
            state,
            q_weight,
            forget_weight,
            input_weight,
            gate_weight,
            out_weight,
            ffn_gate,
            ffn_up,
            ffn_down,
        )
    ]
    layer_out, fv = pl.pallas_call(
        functools.partial(layer, dims),
        out_shape=(
            jax.ShapeDtypeStruct((g, rows, feats), BF16),
            jax.ShapeDtypeStruct((2, rows, cols), F32),
        ),
        in_specs=[VMEM] * 5 + [ANY] * 9,
        out_specs=(VMEM, VMEM),
        scratch_shapes=[
            pltpu.VMEM((2, 2 * feats, cols), BF16),
            pltpu.VMEM((1, 2 * feats, ff), BF16),
            pltpu.VMEM((cols, feats), BF16),
            pltpu.VMEM((ff, feats), BF16),
            pltpu.VMEM((2, n_tp, g, rows, feats), BF16),
            pltpu.VMEM((2, n_tp, g, rows, feats), BF16),
            pltpu.VMEM((n_kv * most, 2 * feats), BF16),
            pltpu.VMEM((2, 2, 1, feats), F32),
            pltpu.VMEM((n_kv, rows, 2 * cols), BF16),
            pltpu.VMEM((n_kv, rows, 2 * cols), BF16),
            pltpu.VMEM((n_kv, rows, ff), BF16),
            pltpu.VMEM((n_kv, rows, ff), BF16),
            pltpu.VMEM((2, 2, rows, cols if square else LANES), BF16),
            pltpu.VMEM((2, 2, rows, ff // 2 if square else LANES), BF16),
            pltpu.VMEM((2, n_kv, rows, LANES), F32),
            pltpu.VMEM((2, half, rows, LANES), F32),
            pltpu.VMEM((rows, cols), F32),
            pltpu.VMEM((rows, cols), F32),
            pltpu.VMEM((rows, heads, size), F32),
            pltpu.VMEM((rows, cols), F32),
            pltpu.VMEM((rows, cols), BF16),
            pltpu.VMEM((n_kv, rows, cols), BF16),
            pltpu.VMEM((rows, ff), BF16),
            pltpu.VMEM((n_kv, rows, ff), BF16),
            pltpu.VMEM((2, n_tp, g, rows, feats), F32),
            pltpu.VMEM((2, n_tp, g, rows, feats), BF16),
            pltpu.VMEM((2, n_tp, g, rows, feats), BF16),
            pltpu.VMEM((g, rows, feats), BF16),
            pltpu.VMEM((SLOTS, chunk, heads, size, size), F32),
            dma((n_sems,)),
            dma((n_sems,)),
            dma((5,)),
            dma((SLOTS,)),
        ],
        compiler_params=pltpu.CompilerParams(
            collective_id=0, has_side_effects=True, vmem_limit_bytes=VMEM_LIMIT
        ),
        name="layer",
    )(*held)
    state_block = pl.BlockSpec((chunk, heads, size, size), lambda c: (c, 0, 0, 0))
    whole = pl.BlockSpec((g, rows, feats), lambda c: (0, 0, 0))
    new_state, layer_out = pl.pallas_call(
        state_step,
        out_shape=(
            jax.ShapeDtypeStruct(state.shape, F32),
            jax.ShapeDtypeStruct((g, rows, feats), BF16),
        ),
        grid=(rows // chunk,),
        in_specs=[pl.BlockSpec((2, chunk, cols), lambda c: (0, c, 0)), whole, state_block],
        out_specs=(state_block, whole),
        compiler_params=pltpu.CompilerParams(
            dimension_semantics=("arbitrary",), vmem_limit_bytes=STATE_LIMIT
        ),
        name="state_step",
    )(fv, layer_out, state)
    return (layer_out.reshape(rows_tp, feats), new_state)


VMEM_LIMIT = 41 * 2**20
STATE_LIMIT = 20 * 2**20


def solution(mesh):
    in_specs = (
        P("tp", "kv"),
        P("kv", "tp", None, None),
        P("kv"),
        P("kv", "tp"),
        P("kv", "tp"),
        P("kv", "tp"),
        P("kv", "tp"),
        P("tp"),
        P(),
        P("tp", "kv"),
        P("kv"),
        P("kv", "tp"),
        P("kv", "tp"),
        P("tp", "kv"),
    )
    out_specs = (P("tp", "kv"), P("kv", "tp", None, None))
    step = functools.partial(body, mesh.shape["kv"], mesh.shape["tp"])
    return jax.shard_map(step, mesh=mesh, in_specs=in_specs, out_specs=out_specs, check_vma=False)
```
